32 devices in a mesh: ep: 16 (over z, y, x), tp: 2 (over core).
Axes of the slice: x: 2, y: 2, z: 4, core: 2. Of those that a mesh axis runs over, the one named last changes fastest.
Arguments:
- tokens: bfloat16 [1024, 2048], P('ep', 'tp'), may hold values from -6 to 6
- sequence_state_real: float32 [1024, 128, 64], P('ep', 'tp'), may hold values from -4 to 4
- sequence_state_imaginary: float32 [1024, 128, 64], P('ep', 'tp'), may hold values from -4 to 4
- mixer_norm_gain: float32 [2048], replicated, may hold values from 0.1 to 1.9
- expert_norm_gain: float32 [2048], replicated, may hold values from 0.1 to 1.9
- rate: float32 [128, 64], P('tp'), may hold values from 0.1 to 4
- freq: float32 [128, 64], P('tp'), may hold values from -3 to 3
- log_group_step: float32 [128], P('tp'), may hold values from -3 to 0
- input_map_real: float32 [128, 64, 16], P('tp'), may hold values from -1 to 1
- input_map_imaginary: float32 [128, 64, 16], P('tp'), may hold values from -1 to 1
- output_map_real: float32 [128, 16, 64], P('tp'), may hold values from -0.75 to 0.75
- output_map_imaginary: float32 [128, 16, 64], P('tp'), may hold values from -0.75 to 0.75
- skip: float32 [2048], P('tp'), may hold values from -4 to 4
- mixer_value_weight: bfloat16 [2048, 2048], P('tp'), may hold values from -0.125 to 0.125
- mixer_gate_weight: bfloat16 [2048, 2048], P('tp'), may hold values from -0.125 to 0.125
- group_router_weight: bfloat16 [2048, 4], replicated, may hold values from -0.125 to 0.125
- expert_router_weight: bfloat16 [2048, 16], replicated, may hold values from -0.125 to 0.125
- dense_blend_weight: float32 [2048], replicated, may hold values from -0.125 to 0.125
- routes: int32 [1024, 2], P('ep'), may hold values from 0 to 15, all different within a row; in each aligned block of 64 rows (0 to 63, 64 to 127, ...) at most 16 rows name the same one
- expert_gate_weight: bfloat16 [16, 2048, 1024], P('ep', None, 'tp'), may hold values from -0.125 to 0.125
- expert_up_weight: bfloat16 [16, 2048, 1024], P('ep', None, 'tp'), may hold values from -0.125 to 0.125
- expert_down_weight: bfloat16 [16, 1024, 2048], P('ep', 'tp'), may hold values from -0.1875 to 0.1875
- shared_gate_weight: bfloat16 [2048, 2048], P('tp', 'ep'), may hold values from -0.125 to 0.125
- shared_up_weight: bfloat16 [2048, 2048], P('tp', 'ep'), may hold values from -0.125 to 0.125
- shared_down_weight: bfloat16 [2048, 2048], P(None, 'tp'), may hold values from -0.125 to 0.125
Outputs:
- result: bfloat16 [1024, 2048], P('ep', 'tp')
- next_re: float32 [1024, 128, 64], P('ep', 'tp')
- next_im: float32 [1024, 128, 64], P('ep', 'tp')
The draws below stay inside these ranges and needn't reach their ends.
Inputs may be any that keep to these rules, and one draw needn't show every extreme that they name: `routes`: each row names 2 different experts. Among the rows of one device no expert is named more than 16 times, and in every draw some expert is named exactly 16 times by some device's rows.
All inputs are finite; a program needn't handle non-finite values.
Results may differ from the reference program's by a relative error of at most 0.017.
Values may be sent and summed in bfloat16 or wider, within the bound.
A program may use at most 128 MiB of HBM per device.

```python
import math
import jax
import jax.numpy as jnp
import numpy as np
from jax import lax

MODEL_WIDTH = 2048
CH = 16
G = 128
P_SIZE = 64
SEQ_DEV = 64
TOKENS = 1024
NG = 4
EXPERT_COUNT = 16
EXPERT_HIDDEN = 1024
FS = 2048
TOPK = 2
CAP = 16
N_EP = 16


def block_levels(key, shape, cuts, least, top_value):
    factor_of, own = 1.0, jax.random.fold_in(key, 6)
    for axis_at, shards_of in cuts:
        steps = jnp.exp(jax.random.uniform(jax.random.fold_in(own, axis_at), (shards_of,), jnp.float32, least / len(cuts), top_value / len(cuts)))
        factor_of = factor_of * jnp.repeat(steps, shape[axis_at] // shards_of).reshape([-1 if axis == axis_at else 1 for axis in range(len(shape))])
    return factor_of


def assign_block(key, own, number, rows, number_of, top, reach, lean):
    sequence = jax.random.permutation(key, number_of)
    crowded, common = load_shares(number_of, rows * top, reach, lean, True), load_shares(number_of, rows * top, reach, lean, False)
    places = jnp.arange(number_of)

    def named(tallies, turn):
        used = int((tallies > 0).sum())
        fixed = max(1, used // 4)
        passed = fixed + (places - fixed + turn * (used - fixed)) % max(1, number_of - fixed)
        return jnp.zeros((number_of,), jnp.int32).at[sequence[jnp.where(places < fixed, places, passed)]].set(jnp.asarray(tallies, jnp.int32))

    tallies = jnp.where(number % 4 == 0, named(crowded, number // 4), named(common, number - number // 4 - 1))
    mixed = jax.random.permutation(jax.random.fold_in(own, 3), number_of)
    donor, sink = mixed[0:number_of // 2 * 2:2], mixed[1:number_of // 2 * 2:2]
    room = jnp.minimum(tallies[donor] - 1, reach - tallies[sink]) // 2
    room = jnp.where((donor == sequence[0]) | (sink == sequence[0]) | (tallies[sink] == 0), 0, jnp.maximum(room, 0))
    passed = jax.random.randint(jax.random.fold_in(own, 4), (number_of // 2,), 0, 1 << 20) % (room + 1)
    tallies = tallies.at[donor].add(-passed).at[sink].add(passed)
    items = jnp.searchsorted(jnp.cumsum(tallies), jnp.arange(rows * top), side="right").astype(jnp.int32)
    table = items.reshape(top, rows).T
    table = table[jax.random.permutation(jax.random.fold_in(own, 1), rows)]
    turn = jax.random.randint(jax.random.fold_in(own, 2), (rows, 1), 0, top)
    return jnp.take_along_axis(table, (jnp.arange(top)[None, :] + turn) % top, axis=1)


def load_shares(amount, total, bound, slope, full):
    loads = [(1 << 20) // math.isqrt(rank ** slope) + 1 for rank in range(1, amount + 1)]
    largest = bound if full else min(bound, max(-(-total // amount), total * loads[0] // sum(loads)))
    least = 1 if total - largest >= amount - 1 else 0
    given, surplus = [largest] + [least] * (amount - 1), total - largest - least * (amount - 1)
    while surplus > 0:
        free = [i for i in range(1, amount) if given[i] < largest] or [i for i in range(1, amount) if given[i] < bound]
        pool, remaining = sum([loads[i] for i in free]), surplus
        for i in free:
            more = min(bound - given[i], max(1, remaining * loads[i] // pool), surplus)
            given[i] = given[i] + more
            surplus = surplus - more
    return np.array(given)


def scatter_about(key, extent, deviation, most, cuts=(), kind=jnp.bfloat16):
    values = jax.random.normal(key, extent, jnp.float32) * deviation
    if len(cuts) > 0:
        values = block_levels(key, extent, cuts, -0.22, 0.18) * values
    return jnp.clip(values, min=-most, max=most).astype(kind)


def setup_inputs(seed: int = 0) -> dict:
    key_list = jax.random.split(jax.random.key(seed), 26)
    tokens = scatter_about(key_list[0], (TOKENS, MODEL_WIDTH), 1.0, 6.0, ((0, 16), (1, 2)))
    sequence_state_real = scatter_about(key_list[1], (TOKENS, G, P_SIZE), 0.5, 4.0, ((0, 16), (1, 2)), jnp.float32)
    sequence_state_imaginary = scatter_about(key_list[2], (TOKENS, G, P_SIZE), 0.5, 4.0, ((0, 16), (1, 2)), jnp.float32)
    mixer_norm_gain = jnp.clip(1.0 + 0.18 * jax.random.normal(key_list[3], (MODEL_WIDTH,), jnp.float32), 0.1, 1.9)
    expert_norm_gain = jnp.clip(1.0 + 0.18 * jax.random.normal(key_list[4], (MODEL_WIDTH,), jnp.float32), 0.1, 1.9)
    rate = jnp.clip(jnp.exp(math.log(4.0) - 3.6888794 * jax.random.uniform(key_list[5], (G, P_SIZE), jnp.float32) ** block_levels(key_list[5], (G, P_SIZE), ((0, 2),), -0.2, 0.2)), 0.1, 4.0)
    freq = jnp.clip(jax.random.uniform(key_list[6], (G, P_SIZE), jnp.float32, -3.0, 3.0) * block_levels(key_list[6], (G, P_SIZE), ((0, 2),), -0.4, 0.0), -3.0, 3.0)
    log_group_step = jnp.clip(-3.0 + 3.0 * jax.random.uniform(key_list[7], (G,), jnp.float32) ** block_levels(key_list[7], (G,), ((0, 2),), -0.2, 0.2), -3.0, 0.0)
    input_map_real = scatter_about(key_list[8], (G, P_SIZE, CH), (2 * CH) ** -0.5, 1.0, ((0, 2),), jnp.float32)
    input_map_imaginary = scatter_about(key_list[9], (G, P_SIZE, CH), (2 * CH) ** -0.5, 1.0, ((0, 2),), jnp.float32)
    output_map_real = scatter_about(key_list[10], (G, CH, P_SIZE), P_SIZE ** -0.5, 0.75, ((0, 2),), jnp.float32)
    output_map_imaginary = scatter_about(key_list[11], (G, CH, P_SIZE), P_SIZE ** -0.5, 0.75, ((0, 2),), jnp.float32)
    skip = scatter_about(key_list[12], (MODEL_WIDTH,), 1.0, 4.0, ((0, 2),), jnp.float32)
    mixer_value_weight = scatter_about(key_list[13], (MODEL_WIDTH, MODEL_WIDTH), MODEL_WIDTH ** -0.5, 0.125, ((0, 2),))
    mixer_gate_weight = scatter_about(key_list[14], (MODEL_WIDTH, MODEL_WIDTH), MODEL_WIDTH ** -0.5, 0.125, ((0, 2),))
    group_router_weight = scatter_about(key_list[15], (MODEL_WIDTH, NG), MODEL_WIDTH ** -0.5, 0.125)
    expert_router_weight = scatter_about(key_list[16], (MODEL_WIDTH, EXPERT_COUNT), MODEL_WIDTH ** -0.5, 0.125)
    dense_blend_weight = scatter_about(key_list[17], (MODEL_WIDTH,), MODEL_WIDTH ** -0.5, 0.125, (), jnp.float32)
    routes_keys = jax.random.split(jax.random.fold_in(key_list[18], 1), TOKENS // SEQ_DEV)
    routes_turns = jax.random.permutation(jax.random.fold_in(key_list[18], 3), TOKENS // SEQ_DEV)
    routes = jax.vmap(lambda own, number: assign_block(jax.random.fold_in(key_list[18], 2), own, number, SEQ_DEV, EXPERT_COUNT, TOPK, CAP, 2))(routes_keys, routes_turns).reshape((TOKENS, TOPK))
    expert_gate_weight = scatter_about(key_list[19], (EXPERT_COUNT, MODEL_WIDTH, EXPERT_HIDDEN), MODEL_WIDTH ** -0.5, 0.125, ((0, 16), (2, 2)))
    expert_up_weight = scatter_about(key_list[20], (EXPERT_COUNT, MODEL_WIDTH, EXPERT_HIDDEN), MODEL_WIDTH ** -0.5, 0.125, ((0, 16), (2, 2)))
    expert_down_weight = scatter_about(key_list[21], (EXPERT_COUNT, EXPERT_HIDDEN, MODEL_WIDTH), EXPERT_HIDDEN ** -0.5, 0.1875, ((0, 16), (1, 2)))
    shared_gate_weight = scatter_about(key_list[22], (MODEL_WIDTH, FS), MODEL_WIDTH ** -0.5, 0.125, ((0, 2), (1, 16)))
    shared_up_weight = scatter_about(key_list[23], (MODEL_WIDTH, FS), MODEL_WIDTH ** -0.5, 0.125, ((0, 2), (1, 16)))
    shared_down_weight = scatter_about(key_list[24], (FS, MODEL_WIDTH), FS ** -0.5, 0.125, ((1, 2),))
    return dict(tokens=tokens, sequence_state_real=sequence_state_real, sequence_state_imaginary=sequence_state_imaginary, mixer_norm_gain=mixer_norm_gain, expert_norm_gain=expert_norm_gain, rate=rate, freq=freq, log_group_step=log_group_step, input_map_real=input_map_real, input_map_imaginary=input_map_imaginary, output_map_real=output_map_real, output_map_imaginary=output_map_imaginary, skip=skip, mixer_value_weight=mixer_value_weight, mixer_gate_weight=mixer_gate_weight, group_router_weight=group_router_weight, expert_router_weight=expert_router_weight, dense_blend_weight=dense_blend_weight, routes=routes, expert_gate_weight=expert_gate_weight, expert_up_weight=expert_up_weight, expert_down_weight=expert_down_weight, shared_gate_weight=shared_gate_weight, shared_up_weight=shared_up_weight, shared_down_weight=shared_down_weight)


EPS = 1e-06
PRECISION_MAX = lax.Precision.HIGHEST

def row_scale(values):
    return lax.rsqrt(lax.optimization_barrier(jnp.mean(values * values, axis=-1, keepdims=True)) + EPS)

def narrow(values):
    return lax.optimization_barrier(values.astype(jnp.bfloat16)).astype(jnp.float32)

def split_product(left, right):
    middle = left.shape[1] // 2
    first = jnp.dot(left[:, :middle], right[:middle], preferred_element_type=jnp.float32)
    second = jnp.dot(left[:, middle:], right[middle:], preferred_element_type=jnp.float32)
    return narrow(first) + narrow(second)

def state_factors(rate, freq, log_group_step, input_map_real, input_map_imaginary):
    step_size = jnp.exp(log_group_step)[:, None]
    magnitude = jnp.exp(-rate * step_size)
    abar_re = magnitude * jnp.cos(freq * step_size)
    abar_im = magnitude * jnp.sin(freq * step_size)
    denom = rate * rate + freq * freq
    shift_re = abar_re - 1.0
    fac_re = (abar_im * freq - shift_re * rate) / denom
    fac_im = -(abar_im * rate + shift_re * freq) / denom
    bbar_re = fac_re[:, :, None] * input_map_real - fac_im[:, :, None] * input_map_imaginary
    bbar_im = fac_re[:, :, None] * input_map_imaginary + fac_im[:, :, None] * input_map_real
    return (abar_re, abar_im, bbar_re, bbar_im)

def state_step(normed, sequence_state_real, sequence_state_imaginary, factors, output_map_real, output_map_imaginary, skip):
    abar_re, abar_im, bbar_re, bbar_im = factors
    groups = abar_re.shape[0]
    inputs = normed.astype(jnp.float32)
    grouped = inputs.reshape(inputs.shape[0], groups, -1)
    drive_re = jnp.einsum('tgc,gpc->tgp', grouped, bbar_re, precision=PRECISION_MAX)
    drive_im = jnp.einsum('tgc,gpc->tgp', grouped, bbar_im, precision=PRECISION_MAX)
    fresh_real = abar_re * sequence_state_real - abar_im * sequence_state_imaginary + drive_re
    fresh_imaginary = abar_re * sequence_state_imaginary + abar_im * sequence_state_real + drive_im
    state_readout = jnp.einsum('dor,zdr->zdo', output_map_real, fresh_real, precision=PRECISION_MAX)
    state_readout = state_readout - jnp.einsum('dor,zdr->zdo', output_map_imaginary, fresh_imaginary, precision=PRECISION_MAX)
    mixed = state_readout.reshape(inputs.shape) + skip * inputs
    return (mixed, fresh_real, fresh_imaginary)

def route_weights(group_logits, expert_logits, routes):
    per_group = expert_logits.shape[1] // group_logits.shape[1]
    group_prob = jax.nn.softmax(group_logits, axis=-1)
    chosen = jnp.take_along_axis(expert_logits, routes, axis=1)
    picked_group = jnp.take_along_axis(group_prob, routes // per_group, axis=1)
    return jax.nn.softmax(chosen, axis=1) * picked_group

def reference(tokens, sequence_state_real, sequence_state_imaginary, mixer_norm_gain, expert_norm_gain, rate, freq, log_group_step, input_map_real, input_map_imaginary, output_map_real, output_map_imaginary, skip, mixer_value_weight, mixer_gate_weight, group_router_weight, expert_router_weight, dense_blend_weight, routes, expert_gate_weight, expert_up_weight, expert_down_weight, shared_gate_weight, shared_up_weight, shared_down_weight):
    float_tokens = tokens.astype(jnp.float32)
    normed = (float_tokens * row_scale(float_tokens) * mixer_norm_gain).astype(jnp.bfloat16)
    factors = state_factors(rate, freq, log_group_step, input_map_real, input_map_imaginary)
    mixed, next_re, next_im = state_step(normed, sequence_state_real, sequence_state_imaginary, factors, output_map_real, output_map_imaginary, skip)
    activated = jax.nn.gelu(mixed).astype(jnp.bfloat16)
    value = split_product(activated, mixer_value_weight)
    gate = split_product(activated, mixer_gate_weight)
    mix = (value * jax.nn.sigmoid(gate)).astype(jnp.bfloat16)
    hidden = (float_tokens + mix.astype(jnp.float32)).astype(jnp.bfloat16)
    hidden_f32 = hidden.astype(jnp.float32)
    inverse = row_scale(hidden_f32)
    scaled = hidden_f32 * expert_norm_gain
    hnorm = (scaled * inverse).astype(jnp.bfloat16)
    group_logits = jnp.dot(scaled, group_router_weight.astype(jnp.float32), precision=PRECISION_MAX) * inverse
    expert_logits = jnp.dot(scaled, expert_router_weight.astype(jnp.float32), precision=PRECISION_MAX) * inverse
    blend_logit = jnp.dot(scaled, dense_blend_weight, precision=PRECISION_MAX) * inverse[:, 0]
    weight = route_weights(group_logits, expert_logits, routes)
    top_count = routes.shape[1]
    width = tokens.shape[1]
    flat_routes = routes.reshape(-1)
    order = jnp.argsort(flat_routes, stable=True).astype(jnp.int32)
    sorted_ids = flat_routes[order]
    expert_ids = jnp.arange(expert_router_weight.shape[1], dtype=jnp.int32)
    starts = jnp.searchsorted(sorted_ids, expert_ids, side='left').astype(jnp.int32)
    ends = jnp.searchsorted(sorted_ids, expert_ids, side='right').astype(jnp.int32)
    limit = N_EP * CAP
    padded = jnp.concatenate([order, jnp.zeros((limit,), jnp.int32)])
    flat_weight = weight.reshape(-1)

    def one_expert(index_value):
        picks = lax.dynamic_slice_in_dim(padded, starts[index_value], limit)
        live = (jnp.arange(limit, dtype=jnp.int32) < ends[index_value] - starts[index_value]).astype(jnp.float32)
        token_rows = hnorm[picks // top_count]
        gate_e = jnp.dot(token_rows, expert_gate_weight[index_value], preferred_element_type=jnp.float32)
        expert_up_rows = jnp.dot(token_rows, expert_up_weight[index_value], preferred_element_type=jnp.float32)
        inner = (jax.nn.silu(gate_e) * expert_up_rows).astype(jnp.bfloat16)
        expert_out = split_product(inner, expert_down_weight[index_value]).astype(jnp.bfloat16).astype(jnp.float32)
        return (expert_out * (flat_weight[picks] * live)[:, None], picks // top_count)
    contrib, targets = lax.map(one_expert, expert_ids)
    routed = jnp.zeros((tokens.shape[0], width), jnp.float32).at[targets.reshape(-1)].add(contrib.reshape(-1, width))
    dense_gate = split_product(hnorm, shared_gate_weight)
    dense_up = split_product(hnorm, shared_up_weight)
    dense_inner = (jax.nn.silu(dense_gate) * dense_up).astype(jnp.bfloat16)
    dense_out = jnp.dot(dense_inner, shared_down_weight, preferred_element_type=jnp.float32)
    result = hidden_f32 + routed + jax.nn.sigmoid(blend_logit)[:, None] * dense_out
    return (result.astype(jnp.bfloat16), next_re, next_im)
```

```python
import functools

import jax
import jax.numpy as jnp
from jax import lax
from jax.experimental import pallas as pl
from jax.experimental.pallas import tpu as pltpu
from jax.sharding import PartitionSpec as P

NG = 4
LANES = 128
MESH = pl.DeviceIdType.MESH
VMEM = pl.BlockSpec(memory_space=pltpu.VMEM)


EPS = 1e-06


def state_factors(rate, freq, log_group_step, input_map_real, input_map_imaginary):
    step_size = jnp.exp(log_group_step)[:, None]
    magnitude = jnp.exp(-rate * step_size)
    abar_re = magnitude * jnp.cos(freq * step_size)
    abar_im = magnitude * jnp.sin(freq * step_size)
    denom = rate * rate + freq * freq
    shift_re = abar_re - 1.0
    fac_re = (abar_im * freq - shift_re * rate) / denom
    fac_im = -(abar_im * rate + shift_re * freq) / denom
    bbar_re = fac_re[:, :, None] * input_map_real - fac_im[:, :, None] * input_map_imaginary
    bbar_im = fac_re[:, :, None] * input_map_imaginary + fac_im[:, :, None] * input_map_real
    return (abar_re, abar_im, bbar_re, bbar_im)


def ep_dims(count):
    bits = count.bit_length() - 1
    if 1 << bits != count:
        return (count, 1, 1)
    return (1 << ((bits + 2) // 3), 1 << ((bits + 1) // 3), 1 << (bits // 3))


def mixer_kernel(
    channels, normed_ref, re_ref, im_ref, ar_ref, ai_ref, br_ref, bi_ref, cr_ref, ci_ref, skip_ref,
    act_ref, nre_ref, nim_ref,
):
    rows, lanes = normed_ref.shape
    groups, states = re_ref.shape[1:]
    u = normed_ref[...].astype(jnp.float32)
    lane = lax.broadcasted_iota(jnp.int32, (groups, lanes), 1)
    group = lax.broadcasted_iota(jnp.int32, (groups, lanes), 0)
    mask = jnp.where((lane >= group * channels) & (lane < group * channels + channels), 1.0, 0.0)
    spread = (u[:, None, :] * mask[None]).reshape(rows * groups, lanes).astype(jnp.bfloat16)
    drive_re = jnp.dot(spread, br_ref[...], preferred_element_type=jnp.float32)
    drive_im = jnp.dot(spread, bi_ref[...], preferred_element_type=jnp.float32)
    a_re, a_im = ar_ref[...][None], ai_ref[...][None]
    s_re, s_im = re_ref[...], im_ref[...]
    n_re = a_re * s_re - a_im * s_im + drive_re.reshape(rows, groups, states)
    n_im = a_re * s_im + a_im * s_re + drive_im.reshape(rows, groups, states)
    nre_ref[...] = n_re
    nim_ref[...] = n_im
    dims = (((1,), (1,)), ((), ()))
    flat_re = n_re.reshape(rows * groups, states).astype(jnp.bfloat16)
    flat_im = n_im.reshape(rows * groups, states).astype(jnp.bfloat16)
    read = lax.dot_general(flat_re, cr_ref[...], dims, preferred_element_type=jnp.float32)
    read = read - lax.dot_general(flat_im, ci_ref[...], dims, preferred_element_type=jnp.float32)
    mixed = jnp.sum(read.reshape(rows, groups, lanes) * mask[None], axis=1) + skip_ref[...] * u
    act_ref[...] = jax.nn.gelu(mixed).astype(jnp.bfloat16)


def mixer(normed, state_re, state_im, factors, out_re, out_im, skip):
    abar_re, abar_im, bbar_re, bbar_im = factors
    rows, width = normed.shape
    groups, states = abar_re.shape
    channels = width // groups
    per = LANES // channels
    maps = [
        jnp.swapaxes(b, 1, 2).reshape(width, states).astype(jnp.bfloat16) for b in (bbar_re, bbar_im)
    ] + [o.reshape(width, states).astype(jnp.bfloat16) for o in (out_re, out_im)]
    cols = pl.BlockSpec((rows, LANES), lambda i: (0, i))
    state = pl.BlockSpec((rows, per, states), lambda i: (0, i, 0))
    abar = pl.BlockSpec((per, states), lambda i: (i, 0))
    chan = pl.BlockSpec((LANES, states), lambda i: (i, 0))
    return pl.pallas_call(
        functools.partial(mixer_kernel, channels),
        grid=(width // LANES,),
        in_specs=[cols, state, state, abar, abar, chan, chan, chan, chan,
                  pl.BlockSpec((1, LANES), lambda i: (0, i))],
        out_specs=[cols, state, state],
        out_shape=[
            jax.ShapeDtypeStruct((rows, width), jnp.bfloat16),
            jax.ShapeDtypeStruct(state_re.shape, jnp.float32),
            jax.ShapeDtypeStruct(state_re.shape, jnp.float32),
        ],
        name="mixer",
    )(normed, state_re, state_im, abar_re, abar_im, *maps, skip[None, :])


def greet(peers):
    barrier = pltpu.get_barrier_semaphore()
    for peer in peers:
        pl.semaphore_signal(barrier, inc=1, device_id=peer, device_id_type=MESH)
    pl.semaphore_wait(barrier, len(peers))


def remote(src, dst, send, recv, peer):
    return pltpu.make_async_remote_copy(
        src_ref=src, dst_ref=dst, send_sem=send, recv_sem=recv, device_id=peer, device_id_type=MESH
    )


def pair_kernel(count, *refs):
    sources, targets, (send, recv) = refs[:count], refs[count:2 * count], refs[2 * count:]
    peer = (lax.axis_index("ep"), 1 - lax.axis_index("tp"))
    greet([peer])
    copies = [remote(s, t, send.at[i], recv.at[i], peer) for i, (s, t) in enumerate(zip(sources, targets))]
    for copy in copies:
        copy.start()
    for copy in copies:
        copy.wait()


def pair_swap(number, *arrays):
    count = len(arrays)
    return pl.pallas_call(
        functools.partial(pair_kernel, count),
        in_specs=[VMEM] * count,
        out_specs=[VMEM] * count,
        out_shape=[jax.ShapeDtypeStruct(a.shape, a.dtype) for a in arrays],
        scratch_shapes=[pltpu.SemaphoreType.DMA((count,))] * 2,
        compiler_params=pltpu.CompilerParams(collective_id=number, has_side_effects=True),
        name="pair_swap",
    )(*arrays)


def gather_plan(units):
    first = units // 8
    second = (units - first + 1) // 2
    return [(0, first, (2, 1, 0)), (first, second, (0, 1, 2)), (first + second, units - first - second, (0, 2, 1))]


def hidden_kernel(
    dims, width, keep_ref, send_ref, tokens_ref, gain_ref, router_ref, ranks_ref,
    hidden_ref, stats_ref, rows_ref, rank_out_ref,
    vg_buf, stat_buf, stat_in, pair_send, pair_recv, send, recv,
):
    ep, tp = lax.axis_index("ep"), lax.axis_index("tp")
    me = (ep // (dims[1] * dims[2]), (ep // dims[2]) % dims[1], ep % dims[2])
    partner = (ep, 1 - tp)

    def neighbour(dim, step):
        c = [me[d] if d != dim else lax.rem(me[d] + step, dims[d]) for d in range(3)]
        return ((c[0] * dims[1] + c[1]) * dims[2] + c[2], tp)

    greet([partner] + [neighbour(d, s) for d in range(3) for s in range(1, dims[d])])
    swap = remote(send_ref, vg_buf, pair_send.at[0], pair_recv.at[0], partner)
    swap.start()
    rank_out_ref[me[0], me[1], me[2]] = ranks_ref[...]
    swap.wait()
    rows, half = tokens_ref.shape
    value = keep_ref[0].astype(jnp.float32) + vg_buf[0].astype(jnp.float32)
    gate = keep_ref[1].astype(jnp.float32) + vg_buf[1].astype(jnp.float32)
    mix = (value * jax.nn.sigmoid(gate)).astype(jnp.bfloat16).astype(jnp.float32)
    hidden = (tokens_ref[...].astype(jnp.float32) + mix).astype(jnp.bfloat16)
    hidden_ref[...] = hidden
    hidden = hidden.astype(jnp.float32)
    scaled = hidden * gain_ref[...]
    raw = jnp.dot(scaled.astype(jnp.bfloat16), router_ref[...], preferred_element_type=jnp.float32)
    squares = jnp.sum(hidden * hidden, axis=1, keepdims=True)
    lane = lax.broadcasted_iota(jnp.int32, raw.shape, 1)
    stat_buf[...] = jnp.where(lane == LANES - 1, squares, raw)
    swap = remote(stat_buf, stat_in, pair_send.at[1], pair_recv.at[1], partner)
    swap.start()
    swap.wait()
    total = stat_buf[...] + stat_in[...]
    inverse = lax.rsqrt(total[:, LANES - 1:] / width + EPS)
    stats_ref[...] = total * inverse
    rows_ref[me[0], me[1], me[2]] = (scaled * inverse).astype(jnp.bfloat16)

    paths = [(rows_ref, lo * LANES, n * LANES, order) for lo, n, order in gather_plan(half // LANES) if n]
    paths = [(rank_out_ref, 0, LANES, (2, 1, 0))] + paths
    slots = sum(d - 1 for d in dims)
    pending = [[] for _ in paths]
    for stage in range(3):
        for p, (ref, lo, n, order) in enumerate(paths):
            for copy in pending[p]:
                copy.wait_recv()
            dim = order[stage]
            done = order[:stage]
            where = tuple(pl.ds(0, dims[d]) if d in done else pl.ds(me[d], 1) for d in range(3))
            block = ref.at[where + (pl.ds(0, rows), pl.ds(lo, n))]
            base = p * slots + sum(dims[d] - 1 for d in done)
            fresh = [
                remote(block, block, send.at[base + s - 1], recv.at[base + s - 1], neighbour(dim, s))
                for s in range(1, dims[dim])
            ]
            for copy in fresh:
                copy.start()
            for copy in pending[p]:
                copy.wait_send()
            pending[p] = fresh
    for copies in pending:
        for copy in copies:
            copy.wait()


def hidden_rows(dims, width, keep, give, tokens, gain, router, ranks):
    rows, half = tokens.shape
    slots = 4 * sum(d - 1 for d in dims)
    return pl.pallas_call(
        functools.partial(hidden_kernel, dims, width),
        in_specs=[VMEM] * 6,
        out_specs=[VMEM] * 4,
        out_shape=[
            jax.ShapeDtypeStruct((rows, half), jnp.bfloat16),
            jax.ShapeDtypeStruct((rows, LANES), jnp.float32),
            jax.ShapeDtypeStruct(dims + (rows, half), jnp.bfloat16),
            jax.ShapeDtypeStruct(dims + (rows, LANES), jnp.bfloat16),
        ],
        scratch_shapes=[
            pltpu.VMEM((2, rows, half), jnp.bfloat16),
            pltpu.VMEM((rows, LANES), jnp.float32),
            pltpu.VMEM((rows, LANES), jnp.float32),
            pltpu.SemaphoreType.DMA((2,)),
            pltpu.SemaphoreType.DMA((2,)),
            pltpu.SemaphoreType.DMA((slots,)),
            pltpu.SemaphoreType.DMA((slots,)),
        ],
        compiler_params=pltpu.CompilerParams(collective_id=2, has_side_effects=True),
        name="hidden_rows",
    )(keep, give, tokens, gain, router, ranks)


def return_kernel(
    n, keep_ref, give_ref, dense_ref, ret_ref, dense_out_ref,
    got, summed, pair_send, pair_recv, e_send, e_recv, d_send, d_recv, local,
):
    ep, tp = lax.axis_index("ep"), lax.axis_index("tp")
    partner = (ep, 1 - tp)
    peers = [lax.rem(ep + s, n) for s in range(1, n)]
    greet([partner] + [(q, tp) for q in peers])
    swap = remote(give_ref, got, pair_send.at[0], pair_recv.at[0], partner)
    swap.start()
    dense_own = pltpu.make_async_copy(dense_ref.at[ep], dense_out_ref.at[tp, ep], local.at[0])
    dense_own.start()
    dense = [
        remote(dense_ref.at[q], dense_out_ref.at[tp, ep], d_send.at[i], d_recv.at[i], (q, tp))
        for i, q in enumerate(peers)
    ]
    for copy in dense:
        copy.start()
    swap.wait()
    summed[...] = (keep_ref[...].astype(jnp.float32) + got[...].astype(jnp.float32)).astype(jnp.bfloat16)
    own = pltpu.make_async_copy(summed.at[ep], ret_ref.at[ep], local.at[1])
    own.start()
    experts = [
        remote(summed.at[q], ret_ref.at[ep], e_send.at[i], e_recv.at[i], (q, tp))
        for i, q in enumerate(peers)
    ]
    for copy in experts:
        copy.start()
    dense_own.wait()
    for copy in dense:
        copy.wait_recv()
    share = remote(
        dense_out_ref.at[tp], dense_out_ref.at[tp], pair_send.at[1], pair_recv.at[1], partner
    )
    share.start()
    for copy in dense:
        copy.wait_send()
    own.wait()
    for copy in experts:
        copy.wait()
    share.wait()


def return_rows(keep, give, dense):
    n = keep.shape[0]
    dma = pltpu.SemaphoreType.DMA
    return pl.pallas_call(
        functools.partial(return_kernel, n),
        in_specs=[VMEM] * 3,
        out_specs=[VMEM] * 2,
        out_shape=[
            jax.ShapeDtypeStruct(keep.shape, jnp.bfloat16),
            jax.ShapeDtypeStruct((2,) + dense.shape, jnp.bfloat16),
        ],
        scratch_shapes=[
            pltpu.VMEM(keep.shape, jnp.bfloat16),
            pltpu.VMEM(keep.shape, jnp.bfloat16),
            dma((2,)), dma((2,)),
            dma((n - 1,)), dma((n - 1,)), dma((n - 1,)), dma((n - 1,)), dma((2,)),
        ],
        compiler_params=pltpu.CompilerParams(collective_id=3, has_side_effects=True),
        name="return_rows",
    )(keep, give, dense)


def shards(
    ep_count,
    tokens,
    sequence_state_real,
    sequence_state_imaginary,
    mixer_norm_gain,
    expert_norm_gain,
    rate,
    freq,
    log_group_step,
    input_map_real,
    input_map_imaginary,
    output_map_real,
    output_map_imaginary,
    skip,
    mixer_value_weight,
    mixer_gate_weight,
    group_router_weight,
    expert_router_weight,
    dense_blend_weight,
    routes,
    expert_gate_weight,
    expert_up_weight,
    expert_down_weight,
    shared_gate_weight,
    shared_up_weight,
    shared_down_weight,
):
    seq_rows, half_width = tokens.shape
    width = 2 * half_width
    ep, tp = lax.axis_index("ep"), lax.axis_index("tp")
    column_start = tp * half_width

    def own_rows(values):
        return lax.dynamic_slice_in_dim(values, column_start, half_width, 0)

    def own_cols(values, core):
        return lax.dynamic_slice_in_dim(values, core * half_width, half_width, values.ndim - 1)

    experts = expert_router_weight.shape[1]
    top_count = routes.shape[1]
    per_group = experts // NG
    capacity = max(2, 2 * seq_rows * top_count // experts)
    hits = routes[:, :, None] == jnp.arange(experts, dtype=jnp.int32)[None, None, :]
    named = jnp.any(hits, axis=1)
    order = jnp.arange(seq_rows)
    earlier = (order[None, :] <= order[:, None]).astype(jnp.bfloat16)
    counted = jnp.dot(earlier, named.astype(jnp.bfloat16), preferred_element_type=jnp.float32)
    ranks_f32 = jnp.where(named, counted, 0.0)
    ranks = jnp.pad(ranks_f32.astype(jnp.bfloat16), ((0, 0), (0, LANES - experts)))

    float_tokens = tokens.astype(jnp.float32)
    square_sum = lax.psum(jnp.sum(float_tokens * float_tokens, axis=1), "tp")
    first_scale = lax.rsqrt(square_sum / width + EPS)[:, None]
    normed = (float_tokens * first_scale * own_rows(mixer_norm_gain)).astype(jnp.bfloat16)
    factors = state_factors(rate, freq, log_group_step, input_map_real, input_map_imaginary)
    activated, next_re, next_im = mixer(
        normed, sequence_state_real, sequence_state_imaginary, factors,
        output_map_real, output_map_imaginary, skip,
    )
    value_part = jnp.dot(activated, mixer_value_weight, preferred_element_type=jnp.float32)
    gate_part = jnp.dot(activated, mixer_gate_weight, preferred_element_type=jnp.float32)
    stacked = jnp.stack([value_part.astype(jnp.bfloat16), gate_part.astype(jnp.bfloat16)], axis=0)
    router_map = jnp.concatenate(
        [
            own_rows(group_router_weight),
            own_rows(expert_router_weight),
            own_rows(dense_blend_weight).astype(jnp.bfloat16)[:, None],
        ],
        axis=1,
    )
    router_map = jnp.pad(router_map, ((0, 0), (0, LANES - router_map.shape[1])))
    hidden, stats, gathered, gathered_ranks = hidden_rows(
        ep_dims(ep_count), width, own_cols(stacked, tp), own_cols(stacked, 1 - tp), tokens,
        own_rows(expert_norm_gain)[None, :], router_map, ranks,
    )
    rows = gathered.reshape(ep_count * seq_rows, half_width)
    rank_rows = gathered_ranks.reshape(ep_count * seq_rows, LANES)
    lane = jnp.arange(LANES, dtype=jnp.int32)[None, :]
    mine = jnp.sum(jnp.where(lane == ep, rank_rows.astype(jnp.float32), 0.0), axis=1).astype(jnp.int32)
    source = jnp.arange(ep_count * seq_rows, dtype=jnp.int32) // seq_rows
    slot = jnp.where(mine > 0, source * capacity + mine - 1, -1)
    dispatch = slot[None, :] == jnp.arange(ep_count * capacity, dtype=jnp.int32)[:, None]
    half_rows = jnp.dot(
        dispatch.astype(jnp.bfloat16), rows, preferred_element_type=jnp.float32
    ).astype(jnp.bfloat16)

    half_seq = seq_rows // 2
    dense_cols = shared_gate_weight.shape[1]
    dense_part = jnp.stack(
        [
            jnp.dot(rows, w, preferred_element_type=jnp.float32).astype(jnp.bfloat16)
            for w in (shared_gate_weight, shared_up_weight)
        ]
    ).reshape(2, ep_count, 2, half_seq, dense_cols)

    def token_half(core):
        return lax.dynamic_index_in_dim(dense_part, core, 2, keepdims=False)

    other_rows, dense_got = pair_swap(1, half_rows, token_half(1 - tp))
    dense_sum = token_half(tp).astype(jnp.float32) + dense_got.astype(jnp.float32)
    dense_inner = (jax.nn.silu(dense_sum[0]) * dense_sum[1]).astype(jnp.bfloat16)

    first_rows = jnp.where(tp == 0, half_rows, other_rows)
    second_rows = jnp.where(tp == 0, other_rows, half_rows)
    token_rows = jnp.concatenate([first_rows, second_rows], axis=1)
    gate_e = jnp.dot(token_rows, expert_gate_weight[0], preferred_element_type=jnp.float32)
    up_e = jnp.dot(token_rows, expert_up_weight[0], preferred_element_type=jnp.float32)
    inner = (jax.nn.silu(gate_e) * up_e).astype(jnp.bfloat16)
    part_out = jnp.dot(inner, expert_down_weight[0], preferred_element_type=jnp.float32).astype(jnp.bfloat16)
    part_out = part_out.reshape(ep_count, capacity, width)
    returned, dense_all = return_rows(own_cols(part_out, tp), own_cols(part_out, 1 - tp), dense_inner)

    logits, blend_logit = stats[:, :NG + experts], stats[:, NG + experts]
    group_prob = jax.nn.softmax(logits[:, :NG], axis=-1)
    chosen = jnp.sum(jnp.where(hits, logits[:, None, NG:], 0.0), axis=2)
    group_hits = (routes // per_group)[:, :, None] == jnp.arange(NG, dtype=jnp.int32)[None, None, :]
    group_sel = jnp.sum(jnp.where(group_hits, group_prob[:, None, :], 0.0), axis=2)
    weights = jax.nn.softmax(chosen, axis=1) * group_sel
    expert_weight = jnp.sum(jnp.where(hits, weights[:, :, None], 0.0), axis=1)
    places = jnp.arange(capacity, dtype=jnp.float32) + 1.0
    combine = jnp.where(ranks_f32[:, :, None] == places[None, None, :], expert_weight[:, :, None], 0.0)
    combine = combine.reshape(seq_rows, experts * capacity).astype(jnp.bfloat16)
    routed = jnp.dot(
        combine, returned.reshape(experts * capacity, half_width), preferred_element_type=jnp.float32
    )
    dense_rows = jnp.transpose(dense_all, (0, 2, 1, 3)).reshape(seq_rows, ep_count * dense_cols)
    dense_out = jnp.dot(dense_rows, shared_down_weight, preferred_element_type=jnp.float32)
    result = hidden.astype(jnp.float32) + routed + jax.nn.sigmoid(blend_logit)[:, None] * dense_out
    return (result.astype(jnp.bfloat16), next_re, next_im)


def solution(mesh):
    placed = (
        P("ep", "tp"),
        P("ep", "tp", None),
        P("ep", "tp", None),
        P(),
        P(),
        P("tp", None),
        P("tp", None),
        P("tp"),
        P("tp", None, None),
        P("tp", None, None),
        P("tp", None, None),
        P("tp", None, None),
        P("tp"),
        P("tp", None),
        P("tp", None),
        P(),
        P(),
        P(),
        P("ep", None),
        P("ep", None, "tp"),
        P("ep", None, "tp"),
        P("ep", "tp", None),
        P("tp", "ep"),
        P("tp", "ep"),
        P(None, "tp"),
    )
    return jax.shard_map(
        functools.partial(shards, mesh.shape["ep"]),
        mesh=mesh,
        in_specs=placed,
        out_specs=(P("ep", "tp"), P("ep", "tp", None), P("ep", "tp", None)),
        check_vma=False,
    )
```

```python
import functools

import jax
import jax.numpy as jnp
from jax import lax
from jax.experimental import pallas as pl
from jax.experimental.pallas import tpu as pltpu
from jax.sharding import PartitionSpec as P

NG = 4
LANES = 128
MESH = pl.DeviceIdType.MESH
VMEM = pl.BlockSpec(memory_space=pltpu.VMEM)


EPS = 1e-06


def state_factors(rate, freq, log_group_step, input_map_real, input_map_imaginary):
    step_size = jnp.exp(log_group_step)[:, None]
    magnitude = jnp.exp(-rate * step_size)
    abar_re = magnitude * jnp.cos(freq * step_size)
    abar_im = magnitude * jnp.sin(freq * step_size)
    denom = rate * rate + freq * freq
    shift_re = abar_re - 1.0
    fac_re = (abar_im * freq - shift_re * rate) / denom
    fac_im = -(abar_im * rate + shift_re * freq) / denom
    bbar_re = fac_re[:, :, None] * input_map_real - fac_im[:, :, None] * input_map_imaginary
    bbar_im = fac_re[:, :, None] * input_map_imaginary + fac_im[:, :, None] * input_map_real
    return (abar_re, abar_im, bbar_re, bbar_im)


def ep_dims(count):
    bits = count.bit_length() - 1
    if 1 << bits != count:
        return (count, 1, 1)
    return (1 << ((bits + 2) // 3), 1 << ((bits + 1) // 3), 1 << (bits // 3))


def mixer_kernel(
    channels, normed_ref, re_ref, im_ref, ar_ref, ai_ref, br_ref, bi_ref, cr_ref, ci_ref, skip_ref,
    act_ref, nre_ref, nim_ref,
):
    rows, lanes = normed_ref.shape
    groups, states = re_ref.shape[1:]
    u = normed_ref[...].astype(jnp.float32)
    lane = lax.broadcasted_iota(jnp.int32, (groups, lanes), 1)
    group = lax.broadcasted_iota(jnp.int32, (groups, lanes), 0)
    mask = jnp.where((lane >= group * channels) & (lane < group * channels + channels), 1.0, 0.0)
    spread = (u[:, None, :] * mask[None]).reshape(rows * groups, lanes).astype(jnp.bfloat16)
    drive_re = jnp.dot(spread, br_ref[...], preferred_element_type=jnp.float32)
    drive_im = jnp.dot(spread, bi_ref[...], preferred_element_type=jnp.float32)
    a_re, a_im = ar_ref[...][None], ai_ref[...][None]
    s_re, s_im = re_ref[...], im_ref[...]
    n_re = a_re * s_re - a_im * s_im + drive_re.reshape(rows, groups, states)
    n_im = a_re * s_im + a_im * s_re + drive_im.reshape(rows, groups, states)
    nre_ref[...] = n_re
    nim_ref[...] = n_im
    dims = (((1,), (1,)), ((), ()))
    flat_re = n_re.reshape(rows * groups, states).astype(jnp.bfloat16)
    flat_im = n_im.reshape(rows * groups, states).astype(jnp.bfloat16)
    read = lax.dot_general(flat_re, cr_ref[...].astype(jnp.bfloat16), dims, preferred_element_type=jnp.float32)
    read = read - lax.dot_general(flat_im, ci_ref[...].astype(jnp.bfloat16), dims, preferred_element_type=jnp.float32)
    mixed = jnp.sum(read.reshape(rows, groups, lanes) * mask[None], axis=1) + skip_ref[...] * u
    act_ref[...] = jax.nn.gelu(mixed).astype(jnp.bfloat16)


def mixer(normed, state_re, state_im, factors, out_re, out_im, skip):
    abar_re, abar_im, bbar_re, bbar_im = factors
    rows, width = normed.shape
    groups, states = abar_re.shape
    channels = width // groups
    per = LANES // channels
    maps = [
        jnp.swapaxes(b, 1, 2).reshape(width, states).astype(jnp.bfloat16) for b in (bbar_re, bbar_im)
    ] + [o.reshape(width, states) for o in (out_re, out_im)]
    cols = pl.BlockSpec((rows, LANES), lambda i: (0, i))
    state = pl.BlockSpec((rows, per, states), lambda i: (0, i, 0))
    abar = pl.BlockSpec((per, states), lambda i: (i, 0))
    chan = pl.BlockSpec((LANES, states), lambda i: (i, 0))
    return pl.pallas_call(
        functools.partial(mixer_kernel, channels),
        grid=(width // LANES,),
        in_specs=[cols, state, state, abar, abar, chan, chan, chan, chan,
                  pl.BlockSpec((1, LANES), lambda i: (0, i))],
        out_specs=[cols, state, state],
        out_shape=[
            jax.ShapeDtypeStruct((rows, width), jnp.bfloat16),
            jax.ShapeDtypeStruct(state_re.shape, jnp.float32),
            jax.ShapeDtypeStruct(state_re.shape, jnp.float32),
        ],
        name="mixer",
    )(normed, state_re, state_im, abar_re, abar_im, *maps, skip[None, :])


def greet(peers):
    barrier = pltpu.get_barrier_semaphore()
    for peer in peers:
        pl.semaphore_signal(barrier, inc=1, device_id=peer, device_id_type=MESH)
    pl.semaphore_wait(barrier, len(peers))


def remote(src, dst, send, recv, peer):
    return pltpu.make_async_remote_copy(
        src_ref=src, dst_ref=dst, send_sem=send, recv_sem=recv, device_id=peer, device_id_type=MESH
    )


def pair_kernel(count, *refs):
    sources, targets, (send, recv) = refs[:count], refs[count:2 * count], refs[2 * count:]
    peer = (lax.axis_index("ep"), 1 - lax.axis_index("tp"))
    greet([peer])
    copies = [remote(s, t, send.at[i], recv.at[i], peer) for i, (s, t) in enumerate(zip(sources, targets))]
    for copy in copies:
        copy.start()
    for copy in copies:
        copy.wait()


def pair_swap(number, *arrays):
    count = len(arrays)
    return pl.pallas_call(
        functools.partial(pair_kernel, count),
        in_specs=[VMEM] * count,
        out_specs=[VMEM] * count,
        out_shape=[jax.ShapeDtypeStruct(a.shape, a.dtype) for a in arrays],
        scratch_shapes=[pltpu.SemaphoreType.DMA((count,))] * 2,
        compiler_params=pltpu.CompilerParams(collective_id=number, has_side_effects=True),
        name="pair_swap",
    )(*arrays)


def gather_plan(units):
    first = units // 8
    second = (units - first + 1) // 2
    return [(0, first, (2, 1, 0)), (first, second, (0, 1, 2)), (first + second, units - first - second, (0, 2, 1))]


def hidden_kernel(
    dims, width, keep_ref, send_ref, tokens_ref, gain_ref, group_ref, expert_ref, blend_ref, ranks_ref, named_ref,
    hidden_ref, stats_ref, rows_ref, rank_out_ref,
    vg_buf, router, stat_buf, stat_in, pair_send, pair_recv, send, recv,
):
    ep, tp = lax.axis_index("ep"), lax.axis_index("tp")
    me = (ep // (dims[1] * dims[2]), (ep // dims[2]) % dims[1], ep % dims[2])
    partner = (ep, 1 - tp)
    rows, half = tokens_ref.shape
    experts = expert_ref.shape[0]
    paths = [(rows_ref, lo * LANES, n * LANES, order) for lo, n, order in gather_plan(half // LANES) if n]
    paths = [(rank_out_ref, 0, LANES, (2, 1, 0))] + paths

    def neighbour(dim, step):
        c = [me[d] if d != dim else lax.rem(me[d] + step, dims[d]) for d in range(3)]
        return ((c[0] * dims[1] + c[1]) * dims[2] + c[2], tp)

    sent = {}

    def give(p, level, *offsets):
        ref, lo, n, order = paths[p]
        spot = list(me)
        for d, o in zip(order, offsets):
            spot[d] = lax.rem(me[d] + dims[d] - o, dims[d])
        block = ref.at[spot[0], spot[1], spot[2], :, pl.ds(lo, n)]
        for step in range(1, dims[order[level]]):
            key = (p,) + offsets + (step,)
            at = len(sent)
            copy = remote(block, block, send.at[at], recv.at[at], neighbour(order[level], step))
            copy.start()
            sent[key] = copy

    greet([partner] + [neighbour(d, s) for d in range(3) for s in range(1, dims[d])])
    swap = remote(send_ref, vg_buf, pair_send.at[0], pair_recv.at[0], partner)
    swap.start()
    rank_out_ref[me[0], me[1], me[2]] = ranks_ref[...]
    mine = pl.ds(pl.multiple_of(tp * half, LANES), half)
    groups = group_ref.shape[0]
    router[...] = jnp.zeros_like(router)
    router[0:experts] = expert_ref[:, mine].astype(jnp.float32)
    router[experts:experts + groups] = group_ref[:, mine].astype(jnp.float32)
    router[experts + groups:experts + groups + 1] = blend_ref[:, mine]
    stat_buf[...] = jnp.zeros_like(stat_buf)
    swap.wait()
    value = keep_ref[0].astype(jnp.float32) + vg_buf[0].astype(jnp.float32)
    gate = keep_ref[1].astype(jnp.float32) + vg_buf[1].astype(jnp.float32)
    mix = (value * jax.nn.sigmoid(gate)).astype(jnp.bfloat16).astype(jnp.float32)
    hidden = (tokens_ref[...].astype(jnp.float32) + mix).astype(jnp.bfloat16)
    hidden_ref[...] = hidden
    hidden = hidden.astype(jnp.float32)
    scaled = hidden * gain_ref[:, mine]
    raw = lax.dot_general(
        scaled.astype(jnp.bfloat16), router[...].astype(jnp.bfloat16), (((1,), (1,)), ((), ())),
        preferred_element_type=jnp.float32,
    )
    stat_buf[:, 0:router.shape[0]] = raw
    stat_buf[:, LANES - 1:LANES] = jnp.sum(hidden * hidden, axis=1, keepdims=True)
    swap = remote(stat_buf, stat_in, pair_send.at[1], pair_recv.at[1], partner)
    swap.start()
    swap.wait()
    total = stat_buf[...] + stat_in[...]
    inverse = lax.rsqrt(total[:, LANES - 1:] / width + EPS)
    rows_ref[me[0], me[1], me[2]] = (scaled * inverse).astype(jnp.bfloat16)

    every = range(len(paths))
    size = [[dims[d] for d in path[3]] for path in paths]
    for p in every:
        give(p, 0)
    for p in every:
        give(p, 1, 0)
    for p in every:
        give(p, 2, 0, 0)
    for p in every:
        for b in range(1, size[p][1]):
            sent[(p, 0, b)].wait_recv()
            give(p, 2, 0, b)
    for a in sorted(range(1, max(dims)), key=lambda o: min(o, max(dims) - o)):
        for p in every:
            if a < size[p][0]:
                sent[(p, a)].wait_recv()
                give(p, 1, a)
                give(p, 2, a, 0)
    for a in sorted(range(1, max(dims)), key=lambda o: min(o, max(dims) - o)):
        for p in every:
            if a < size[p][0]:
                for b in range(1, size[p][1]):
                    sent[(p, a, b)].wait_recv()
                    give(p, 2, a, b)

    logits = total * inverse
    lane = lax.broadcasted_iota(jnp.int32, logits.shape, 1)
    named = named_ref[...] > 0
    is_group = (lane >= experts) & (lane < experts + groups)
    low = jnp.full_like(logits, -jnp.inf)
    group_exp = jnp.exp(logits - jnp.max(jnp.where(is_group, logits, low), axis=1, keepdims=True))
    group_exp = jnp.where(is_group, group_exp, 0.0)
    group_prob = group_exp / jnp.sum(group_exp, axis=1, keepdims=True)
    top = jnp.max(jnp.where(named, logits, low), axis=1, keepdims=True)
    chosen = jnp.where(named, jnp.exp(jnp.where(named, logits - top, 0.0)), 0.0)
    chosen = chosen / jnp.sum(chosen, axis=1, keepdims=True)
    per_group = experts // groups
    spread = jnp.zeros_like(logits)
    for g in range(groups):
        inside = (lane >= g * per_group) & (lane < (g + 1) * per_group)
        spread = jnp.where(inside, group_prob[:, experts + g:experts + g + 1], spread)
    stats_ref[...] = jnp.where(named, chosen * spread, jax.nn.sigmoid(logits))

    for key, copy in sent.items():
        if len(key) == 4:
            copy.wait_recv()
    for copy in sent.values():
        copy.wait_send()


def hidden_rows(dims, width, keep, give, tokens, gain, group_map, expert_map, blend_map, ranks, named):
    rows, half = tokens.shape
    experts = expert_map.shape[0]
    slots = 4 * (dims[0] * dims[1] * dims[2] - 1)
    routers = -(-(experts + group_map.shape[0] + 1) // 8) * 8
    return pl.pallas_call(
        functools.partial(hidden_kernel, dims, width),
        in_specs=[VMEM] * 9,
        out_specs=[VMEM] * 4,
        out_shape=[
            jax.ShapeDtypeStruct((rows, half), jnp.bfloat16),
            jax.ShapeDtypeStruct((rows, LANES), jnp.float32),
            jax.ShapeDtypeStruct(dims + (rows, half), jnp.bfloat16),
            jax.ShapeDtypeStruct(dims + (experts, LANES), jnp.float32),
        ],
        scratch_shapes=[
            pltpu.VMEM((2, rows, half), jnp.bfloat16),
            pltpu.VMEM((routers, half), jnp.float32),
            pltpu.VMEM((rows, LANES), jnp.float32),
            pltpu.VMEM((rows, LANES), jnp.float32),
            pltpu.SemaphoreType.DMA((2,)),
            pltpu.SemaphoreType.DMA((2,)),
            pltpu.SemaphoreType.DMA((slots,)),
            pltpu.SemaphoreType.DMA((slots,)),
        ],
        compiler_params=pltpu.CompilerParams(collective_id=2, has_side_effects=True),
        name="hidden_rows",
    )(keep, give, tokens, gain, group_map, expert_map, blend_map, ranks, named)


def return_kernel(
    n, keep_ref, give_ref, dense_ref, ret_ref, dense_out_ref,
    got, summed, pair_send, pair_recv, e_send, e_recv, d_send, d_recv, local,
):
    ep, tp = lax.axis_index("ep"), lax.axis_index("tp")
    partner = (ep, 1 - tp)
    peers = [lax.rem(ep + s, n) for s in sorted(range(1, n), key=lambda o: abs(2 * o - n))]
    greet([partner] + [(q, tp) for q in peers])
    swap = remote(give_ref, got, pair_send.at[0], pair_recv.at[0], partner)
    swap.start()
    dense_own = pltpu.make_async_copy(dense_ref.at[ep], dense_out_ref.at[tp, ep], local.at[0])
    dense_own.start()
    dense = [
        remote(dense_ref.at[q], dense_out_ref.at[tp, ep], d_send.at[i], d_recv.at[i], (q, tp))
        for i, q in enumerate(peers)
    ]
    for copy in dense:
        copy.start()
    swap.wait()
    summed[...] = (keep_ref[...].astype(jnp.float32) + got[...].astype(jnp.float32)).astype(jnp.bfloat16)
    own = pltpu.make_async_copy(summed.at[ep], ret_ref.at[ep], local.at[1])
    own.start()
    experts = [
        remote(summed.at[q], ret_ref.at[ep], e_send.at[i], e_recv.at[i], (q, tp))
        for i, q in enumerate(peers)
    ]
    for copy in experts:
        copy.start()
    dense_own.wait()
    for copy in dense:
        copy.wait_recv()
    share = remote(
        dense_out_ref.at[tp], dense_out_ref.at[tp], pair_send.at[1], pair_recv.at[1], partner
    )
    share.start()
    for copy in dense:
        copy.wait_send()
    own.wait()
    for copy in experts:
        copy.wait()
    share.wait()


def return_rows(keep, give, dense):
    n = keep.shape[0]
    dma = pltpu.SemaphoreType.DMA
    return pl.pallas_call(
        functools.partial(return_kernel, n),
        in_specs=[VMEM] * 3,
        out_specs=[VMEM] * 2,
        out_shape=[
            jax.ShapeDtypeStruct(keep.shape, jnp.bfloat16),
            jax.ShapeDtypeStruct((2,) + dense.shape, jnp.bfloat16),
        ],
        scratch_shapes=[
            pltpu.VMEM(keep.shape, jnp.bfloat16),
            pltpu.VMEM(keep.shape, jnp.bfloat16),
            dma((2,)), dma((2,)),
            dma((n - 1,)), dma((n - 1,)), dma((n - 1,)), dma((n - 1,)), dma((2,)),
        ],
        compiler_params=pltpu.CompilerParams(collective_id=3, has_side_effects=True),
        name="return_rows",
    )(keep, give, dense)


def shards(
    ep_count,
    tokens,
    sequence_state_real,
    sequence_state_imaginary,
    mixer_norm_gain,
    expert_norm_gain,
    rate,
    freq,
    log_group_step,
    input_map_real,
    input_map_imaginary,
    output_map_real,
    output_map_imaginary,
    skip,
    mixer_value_weight,
    mixer_gate_weight,
    group_router_weight,
    expert_router_weight,
    dense_blend_weight,
    routes,
    expert_gate_weight,
    expert_up_weight,
    expert_down_weight,
    shared_gate_weight,
    shared_up_weight,
    shared_down_weight,
):
    seq_rows, half_width = tokens.shape
    width = 2 * half_width
    ep, tp = lax.axis_index("ep"), lax.axis_index("tp")
    column_start = tp * half_width

    def own_rows(values):
        return lax.dynamic_slice_in_dim(values, column_start, half_width, 0)

    def own_cols(values, core):
        return lax.dynamic_slice_in_dim(values, core * half_width, half_width, values.ndim - 1)

    experts = expert_router_weight.shape[1]
    top_count = routes.shape[1]
    capacity = max(2, 2 * seq_rows * top_count // experts)
    hits = routes[:, :, None] == jnp.arange(experts, dtype=jnp.int32)[None, None, :]
    named = jnp.any(hits, axis=1)
    order = jnp.arange(seq_rows)
    earlier = (order[None, :] <= order[:, None]).astype(jnp.bfloat16)
    counted = jnp.dot(earlier, named.astype(jnp.bfloat16), preferred_element_type=jnp.float32)
    ranks_f32 = jnp.where(named, counted, 0.0)
    ranks = jnp.pad(ranks_f32.T, ((0, 0), (0, LANES - seq_rows)))
    named_lanes = jnp.pad(named.astype(jnp.float32), ((0, 0), (0, LANES - experts)))

    float_tokens = tokens.astype(jnp.float32)
    square_sum = lax.psum(jnp.sum(float_tokens * float_tokens, axis=1), "tp")
    first_scale = lax.rsqrt(square_sum / width + EPS)[:, None]
    normed = (float_tokens * first_scale * own_rows(mixer_norm_gain)).astype(jnp.bfloat16)
    factors = state_factors(rate, freq, log_group_step, input_map_real, input_map_imaginary)
    activated, next_re, next_im = mixer(
        normed, sequence_state_real, sequence_state_imaginary, factors,
        output_map_real, output_map_imaginary, skip,
    )
    value_part = jnp.dot(activated, mixer_value_weight, preferred_element_type=jnp.float32)
    gate_part = jnp.dot(activated, mixer_gate_weight, preferred_element_type=jnp.float32)
    stacked = jnp.stack([value_part.astype(jnp.bfloat16), gate_part.astype(jnp.bfloat16)], axis=0)
    hidden, stats, gathered, gathered_ranks = hidden_rows(
        ep_dims(ep_count), width, own_cols(stacked, tp), own_cols(stacked, 1 - tp), tokens,
        expert_norm_gain[None, :], group_router_weight.T, expert_router_weight.T, dense_blend_weight[None, :],
        ranks, named_lanes,
    )
    rows = gathered.reshape(ep_count * seq_rows, half_width)
    mine = lax.dynamic_index_in_dim(
        gathered_ranks.reshape(ep_count, experts, LANES), ep, 1, keepdims=False
    )[:, :seq_rows].astype(jnp.int32)
    source = jnp.arange(ep_count, dtype=jnp.int32)[:, None]
    slot = jnp.where(mine > 0, source * capacity + mine - 1, -1).reshape(-1)
    dispatch = slot[None, :] == jnp.arange(ep_count * capacity, dtype=jnp.int32)[:, None]
    half_rows = jnp.dot(
        dispatch.astype(jnp.bfloat16), rows, preferred_element_type=jnp.float32
    ).astype(jnp.bfloat16)

    half_seq = seq_rows // 2
    dense_cols = shared_gate_weight.shape[1]
    dense_part = jnp.stack(
        [
            jnp.dot(rows, w, preferred_element_type=jnp.float32).astype(jnp.bfloat16)
            for w in (shared_gate_weight, shared_up_weight)
        ]
    ).reshape(2, ep_count, 2, half_seq, dense_cols)

    def token_half(core):
        return lax.dynamic_index_in_dim(dense_part, core, 2, keepdims=False)

    other_rows, dense_got = pair_swap(1, half_rows, token_half(1 - tp))
    dense_sum = token_half(tp).astype(jnp.float32) + dense_got.astype(jnp.float32)
    dense_inner = (jax.nn.silu(dense_sum[0]) * dense_sum[1]).astype(jnp.bfloat16)

    first_rows = jnp.where(tp == 0, half_rows, other_rows)
    second_rows = jnp.where(tp == 0, other_rows, half_rows)
    token_rows = jnp.concatenate([first_rows, second_rows], axis=1)
    gate_e = jnp.dot(token_rows, expert_gate_weight[0], preferred_element_type=jnp.float32)
    up_e = jnp.dot(token_rows, expert_up_weight[0], preferred_element_type=jnp.float32)
    inner = (jax.nn.silu(gate_e) * up_e).astype(jnp.bfloat16)
    part_out = jnp.dot(inner, expert_down_weight[0], preferred_element_type=jnp.float32).astype(jnp.bfloat16)
    part_out = part_out.reshape(ep_count, capacity, width)
    returned, dense_all = return_rows(own_cols(part_out, tp), own_cols(part_out, 1 - tp), dense_inner)

    expert_weight, blend = stats[:, :experts], stats[:, experts + NG]
    places = jnp.arange(capacity, dtype=jnp.float32) + 1.0
    combine = jnp.where(ranks_f32[:, :, None] == places[None, None, :], expert_weight[:, :, None], 0.0)
    combine = combine.reshape(seq_rows, experts * capacity).astype(jnp.bfloat16)
    routed = jnp.dot(
        combine, returned.reshape(experts * capacity, half_width), preferred_element_type=jnp.float32
    )
    dense_rows = jnp.transpose(dense_all, (0, 2, 1, 3)).reshape(seq_rows, ep_count * dense_cols)
    dense_out = jnp.dot(dense_rows, shared_down_weight, preferred_element_type=jnp.float32)
    result = hidden.astype(jnp.float32) + routed + blend[:, None] * dense_out
    return (result.astype(jnp.bfloat16), next_re, next_im)


def solution(mesh):
    placed = (
        P("ep", "tp"),
        P("ep", "tp", None),
        P("ep", "tp", None),
        P(),
        P(),
        P("tp", None),
        P("tp", None),
        P("tp"),
        P("tp", None, None),
        P("tp", None, None),
        P("tp", None, None),
        P("tp", None, None),
        P("tp"),
        P("tp", None),
        P("tp", None),
        P(),
        P(),
        P(),
        P("ep", None),
        P("ep", None, "tp"),
        P("ep", None, "tp"),
        P("ep", "tp", None),
        P("tp", "ep"),
        P("tp", "ep"),
        P(None, "tp"),
    )
    return jax.shard_map(
        functools.partial(shards, mesh.shape["ep"]),
        mesh=mesh,
        in_specs=placed,
        out_specs=(P("ep", "tp"), P("ep", "tp", None), P("ep", "tp", None)),
        check_vma=False,
    )
```
